128 devices in a mesh: sp: 32 (over z, y, core), tp: 4 (over x).
Axes of the slice: x: 4, y: 4, z: 4, core: 2. Of those that a mesh axis runs over, the one named last changes fastest.
Arguments:
- layer_input: bfloat16 [32768, 2048], P('sp'), may hold values from -6 to 6
- query_weight: bfloat16 [2048, 1024], P(None, 'tp'), may hold values from -0.125 to 0.125
- key_weight: bfloat16 [2048, 1024], P(None, 'tp'), may hold values from -0.125 to 0.125
- value_weight: bfloat16 [2048, 1024], P(None, 'tp'), may hold values from -0.125 to 0.125
- outgate_weight: bfloat16 [2048, 1024], P(None, 'tp'), may hold values from -0.125 to 0.125
- ingate_weight: bfloat16 [2048, 8], replicated, may hold values from -12 to 12, as said below
- forget_weight: bfloat16 [2048, 8], replicated, may hold values from -0.125 to 0.125
- forget_bias: float32 [8], P('tp'), as said below
- forget_shift: float32 [256, 8], P('sp', 'tp'), may hold values from -1 to 1
- init_state: float32 [8, 128, 128], P('tp'), may hold values from -96 to 96
- head_gain: float32 [1024], P('tp'), may hold values from 0.1 to 1.9
- conv_gate_weight: bfloat16 [2048, 1024], P(None, 'tp'), may hold values from -0.125 to 0.125
- conv_input_weight: bfloat16 [2048, 1024], P(None, 'tp'), may hold values from -0.125 to 0.125
- conv_outgate_weight: bfloat16 [2048, 1024], P(None, 'tp'), may hold values from -0.125 to 0.125
- conv_taps: float32 [3, 1024], P(None, 'tp'), may hold values from -3.5 to 3.5
- memory_out_weight: bfloat16 [1024, 2048], replicated, may hold values from -0.125 to 0.125
- conv_out_weight: bfloat16 [1024, 2048], replicated, may hold values from -0.125 to 0.125
Outputs:
- mixed: bfloat16 [32768, 2048], P(('sp', 'tp'))
The draws below stay inside these ranges and needn't reach their ends.
Inputs may be any that keep to these rules, and one draw needn't show every extreme that they name: `forget_bias`: every head's forget offset is at least 3. `ingate_weight`: the columns' scales may differ from head to head.
All inputs are finite; a program needn't handle non-finite values.
Results may differ from the reference program's by a relative error of at most 0.012.
The reference program's roundings to bfloat16 on the way (of `weights`, `memory_out`, `conv_in` and `conv_out`) count: a program that leaves them out, or rounds other values in their place, can miss the bound.
Values may be sent and summed in bfloat16 or wider, within the bound.
A program may use at most 128 MiB of HBM per device.

```python
import jax
import jax.numpy as jnp
from jax import lax

D = 2048
HEADS = 8
DH = 128
CONV_CH = 1024
WIDTH = 3
BLOCK = 128
TOKENS = 32768


def draw_forget_bias(key, part):
    subkeys = jax.random.split(jax.random.fold_in(key, 11), 3)
    slow = jnp.log(jnp.float32(TOKENS)) + jax.random.uniform(subkeys[0], (HEADS,), jnp.float32, 0.0, 1.0)
    fast = jax.random.uniform(subkeys[1], (HEADS,), jnp.float32, 3.0, 4.0)
    order = jax.random.permutation(subkeys[2], HEADS)
    result = jnp.where(order < HEADS // 2, fast, slow)
    return result


def draw_ingate_weight(key, part):
    subkeys = jax.random.split(jax.random.fold_in(key, 23), 1)
    base = jax.random.normal(subkeys[0], (D, HEADS), jnp.float32) * D ** (-0.5)
    result = jnp.clip(base, -12.0, 12.0)
    return result.astype(jnp.bfloat16)


def level_of(stream_key, shape, cuts, smallest, high):
    gain = 1.0
    for dim, parts in cuts:
        heights = jax.random.uniform(jax.random.fold_in(jax.random.fold_in(stream_key, 6), dim), (parts,), jnp.float32, smallest / len(cuts), high / len(cuts))
        gain = gain * jnp.repeat(jnp.exp(heights), shape[dim] // parts).reshape((-1,) + (1,) * (len(shape) - 1 - dim))
    return gain


def gaussian(stream_key, extent, deviation, bound, pieces=(), kind=jnp.bfloat16):
    loudness = level_of(stream_key, extent, pieces, -0.22, 0.18) if pieces else 1.0
    values = jax.random.normal(stream_key, extent, jnp.float32) * deviation * loudness
    return jnp.minimum(jnp.maximum(values, -bound), bound).astype(kind)


def setup_inputs(seed: int = 0) -> dict:
    key_of = jax.random.split(jax.random.key(seed), 18)
    return {
        "layer_input": gaussian(key_of[0], (TOKENS, D), 1.0, 6.0, ((0, 32),)),
        "query_weight": gaussian(key_of[1], (D, HEADS * DH), D ** -0.5, 0.125, ((1, 4),)),
        "key_weight": gaussian(key_of[2], (D, HEADS * DH), D ** -0.5, 0.125, ((1, 4),)),
        "value_weight": gaussian(key_of[3], (D, HEADS * DH), D ** -0.5, 0.125, ((1, 4),)),
        "outgate_weight": gaussian(key_of[4], (D, HEADS * DH), D ** -0.5, 0.125, ((1, 4),)),
        "ingate_weight": draw_ingate_weight(jax.random.fold_in(key_of[17], 71), 0),
        "forget_weight": gaussian(key_of[6], (D, HEADS), D ** -0.5, 0.125),
        "forget_bias": draw_forget_bias(jax.random.fold_in(key_of[17], 71), 0),
        "forget_shift": jnp.clip(jax.random.uniform(key_of[8], (TOKENS // BLOCK, HEADS), jnp.float32, -1.0, 1.0) * level_of(key_of[8], (TOKENS // BLOCK, HEADS), ((0, 32), (1, 4)), -0.4, 0.0), -1.0, 1.0),
        "init_state": gaussian(key_of[9], (HEADS, DH, DH), 16.0, 96.0, ((0, 4),), jnp.float32),
        "head_gain": jnp.clip(1.0 + 0.18 * jax.random.normal(key_of[10], (HEADS * DH,), jnp.float32), 0.1, 1.9),
        "conv_gate_weight": gaussian(key_of[11], (D, CONV_CH), D ** -0.5, 0.125, ((1, 4),)),
        "conv_input_weight": gaussian(key_of[12], (D, CONV_CH), D ** -0.5, 0.125, ((1, 4),)),
        "conv_outgate_weight": gaussian(key_of[13], (D, CONV_CH), D ** -0.5, 0.125, ((1, 4),)),
        "conv_taps": gaussian(key_of[14], (WIDTH, CONV_CH), WIDTH ** -0.5, 3.5, ((1, 4),), jnp.float32),
        "memory_out_weight": gaussian(key_of[15], (HEADS * DH, D), (HEADS * DH + CONV_CH) ** -0.5, 0.125),
        "conv_out_weight": gaussian(key_of[16], (CONV_CH, D), (HEADS * DH + CONV_CH) ** -0.5, 0.125),
    }


norm_eps = 1e-05

def reference(layer_input, query_weight, key_weight, value_weight, outgate_weight, ingate_weight, forget_weight, forget_bias, forget_shift, init_state, head_gain, conv_gate_weight, conv_input_weight, conv_outgate_weight, conv_taps, memory_out_weight, conv_out_weight):
    rescale_factor = DH ** (-0.5)
    highest_value = lax.Precision.HIGHEST

    def project(weight):
        return jnp.dot(layer_input, weight, preferred_element_type=jnp.float32)

    def stored(weight):
        return lax.optimization_barrier(project(weight).astype(jnp.bfloat16))
    query_proj = stored(query_weight)
    key_proj = stored(key_weight)
    value_proj = stored(value_weight)
    out_gate = stored(outgate_weight)
    in_gate = project(ingate_weight)
    forget_logits = project(forget_weight) + forget_bias[None, :] + jnp.repeat(forget_shift, BLOCK, axis=0)
    blocks = TOKENS // BLOCK
    block_shape = (blocks, BLOCK, HEADS, DH)
    query_blocks = query_proj.reshape(block_shape).astype(jnp.float32)
    key_blocks = key_proj.reshape(block_shape).astype(jnp.float32)
    value_blocks = value_proj.reshape(block_shape).astype(jnp.float32)
    gate_blocks = in_gate.reshape(blocks, BLOCK, HEADS)
    forget_blocks = jax.nn.log_sigmoid(forget_logits).reshape(blocks, BLOCK, HEADS)
    causal = jnp.tril(jnp.ones((BLOCK, BLOCK), dtype=bool))

    def advance(state_pair, inputs):
        previous_state, prev_max = state_pair
        local_query, local_key, local_value, gate_here, forget_here = inputs
        cumulative = jnp.cumsum(forget_here, axis=0)
        block_decay = cumulative[-1]
        decay_rows = cumulative.T
        carry_log_values = decay_rows + prev_max[:, None]
        pair_logs = jnp.where(causal[None], decay_rows[:, :, None] - decay_rows[:, None, :] + gate_here.T[:, None, :], -1e+30)
        row_maximum = jnp.maximum(carry_log_values, pair_logs.max(-1))
        scores = jnp.einsum('jhd,shd->hjs', local_query, local_key, precision=highest_value) * rescale_factor
        weights = lax.optimization_barrier((scores * jnp.exp(pair_logs - row_maximum[..., None])).astype(jnp.bfloat16)).astype(jnp.float32)
        inner_part = jnp.einsum('hjs,shv->jhv', weights, local_value, precision=highest_value)
        carried_over = jnp.einsum('reb,ebt->ret', local_query, previous_state, precision=highest_value) * jnp.exp(carry_log_values - row_maximum).T[..., None]
        end_logs = block_decay[None] - cumulative + gate_here
        local_max = end_logs.max(0)
        final_weights = jnp.exp(end_logs - local_max[None])
        state_within = jnp.einsum('glt,glu->ltu', local_key * (rescale_factor * final_weights)[..., None], local_value, precision=highest_value)
        joint_max = jnp.maximum(block_decay + prev_max, local_max)
        joint_state = jnp.exp(block_decay + prev_max - joint_max)[:, None, None] * previous_state + jnp.exp(local_max - joint_max)[:, None, None] * state_within
        return ((joint_state, joint_max), inner_part + carried_over)
    outcome = lax.scan(advance, (init_state, jnp.zeros((HEADS,), jnp.float32)), (query_blocks, key_blocks, value_blocks, gate_blocks, forget_blocks))
    hidden = outcome[1].reshape(TOKENS, HEADS, DH)
    center = hidden.mean(-1, keepdims=True)
    spread = jnp.square(hidden - center).mean(-1, keepdims=True)
    normed = (hidden - center) * lax.rsqrt(spread + norm_eps) * head_gain.reshape(HEADS, DH)
    memory_out = (jax.nn.sigmoid(out_gate.astype(jnp.float32)) * normed.reshape(TOKENS, HEADS * DH)).astype(jnp.bfloat16)
    conv_gate = stored(conv_gate_weight)
    conv_input = stored(conv_input_weight)
    conv_outgate = stored(conv_outgate_weight)
    conv_in = conv_gate * conv_input
    padded = jnp.concatenate([jnp.zeros((WIDTH - 1, CONV_CH), jnp.bfloat16), conv_in], axis=0)
    convolved = conv_taps[0][None, :] * padded[0:TOKENS].astype(jnp.float32)
    for offset in range(1, WIDTH):
        convolved = convolved + conv_taps[offset][None, :] * padded[offset:offset + TOKENS].astype(jnp.float32)
    conv_out = (conv_outgate.astype(jnp.float32) * convolved).astype(jnp.bfloat16)
    total_out = jnp.dot(memory_out, memory_out_weight, preferred_element_type=jnp.float32) + jnp.dot(conv_out, conv_out_weight, preferred_element_type=jnp.float32)
    return total_out.astype(jnp.bfloat16)
```

```python
import functools

import jax
import jax.numpy as jnp
from jax import lax
from jax.experimental import pallas as pl
from jax.experimental.pallas import tpu as pltpu
from jax.sharding import Mesh
from jax.sharding import PartitionSpec as P

F32, BF16 = jnp.float32, jnp.bfloat16
MESH = pl.DeviceIdType.MESH
BLOCK = 128
EPS = 1e-05
LOW = -1e30
TAIL = 16
AXES = ("z", "y", "c", "tp")


def mm(a, b):
    return jnp.dot(a, b, preferred_element_type=F32)


def mm_nt(a, b):
    return lax.dot_general(a, b, (((1,), (1,)), ((), ())), preferred_element_type=F32)


def merge(earlier, latter):
    e_s, e_m, e_d = earlier
    l_s, l_m, l_d = latter
    top = jnp.maximum(l_d + e_m, l_m)
    return jnp.exp(l_d + e_m - top) * e_s + jnp.exp(l_m - top) * l_s, top, e_d + l_d


def pick(cond, a, b):
    return tuple(jnp.where(cond, u, v) for u, v in zip(a, b))


def thirds(v):
    hi = v.astype(BF16).astype(F32)
    mid = (v - hi).astype(BF16).astype(F32)
    return hi, mid, v - hi - mid


def pack(ref, triple):
    s, m, d = triple
    dk, lanes = s.shape
    row = lax.broadcasted_iota(jnp.int32, (TAIL, lanes), 0)
    tail = jnp.zeros((TAIL, lanes), F32)
    for k, part in enumerate((*thirds(m), *thirds(d))):
        tail = jnp.where(row == k, part, tail)
    ref[0:dk, :] = s.astype(BF16)
    ref[dk : dk + TAIL, :] = tail.astype(BF16)


def unpack(ref):
    dk = ref.shape[0] - TAIL
    tail = ref[dk : dk + TAIL, :].astype(F32)
    m = tail[0:1] + tail[1:2] + tail[2:3]
    d = tail[3:4] + tail[4:5] + tail[5:6]
    return ref[0:dk, :].astype(F32), m, d


def kernel(sizes, *refs):
    nz, ny, nc, nt = sizes
    (x_hbm, wk_hbm, wv_hbm, wcg_hbm, wci_hbm, wco_hbm, wq_hbm, wog_hbm, wi_hbm, wf_hbm,
     fb, fs, init_hbm, gain_hbm, taps_hbm, wmo_hbm, wcout_hbm, out_v) = refs[:18]
    (x_v, w_v, wi_v, wf_v, init_v, gain_v, taps_v, wmo_v, wcout_v,
     k_v, v_v, q_v, co_v, og_v, cin_v, hloc_v, acc_v,
     gt_v, rows_v, col_v, fac_v, vt_v, pref_v, bd_v,
     edge_v, halo_v, msg_v, ry_v, msgr_v, rz_v, zs_v, zmd_v, msg4_v, r4_v, ah_v, ahmd_v,
     csend_v, crow_v, msend_v, mrow_v,
     ld_sem, one_send, one_recv, y_send, y_recv, z_send, z_recv,
     c_send, c_recv, m_send, m_recv) = refs[18:]

    z, y, c, t = (lax.axis_index(a) for a in AXES)
    n_sp = nz * ny * nc
    sp = (z * ny + y) * nc + c

    def at_sp(index):
        return {"z": lax.div(index, ny * nc), "y": lax.rem(lax.div(index, nc), ny), "c": lax.rem(index, nc)}

    after = at_sp(lax.rem(sp + 1, n_sp))
    before = at_sp(lax.rem(sp + n_sp - 1, n_sp))
    tokens = x_v.shape[0]
    part = tokens // nt
    nb = tokens // BLOCK
    width = k_v.shape[1]
    heads = width // BLOCK
    dh = BLOCK
    scale = dh ** -0.5
    per = part // BLOCK
    near = sorted(range(1, nt), key=lambda d: -min(d, nt - d))
    plane = [(dy, dc) for dy in (*sorted(range(1, ny), key=lambda d: -min(d, ny - d)), 0) for dc in range(nc) if dy or dc]

    def chunk(r):
        return pl.ds(r * part, part)

    loads = {}

    def load(name, src, dst):
        copy = pltpu.make_async_copy(src, dst, ld_sem.at[len(loads)])
        copy.start()
        loads[name] = copy

    def need(*names):
        for name in names:
            loads[name].wait()

    load("x0", x_hbm.at[chunk(0)], x_v.at[chunk(0)])
    load("k", wk_hbm, w_v.at[0])
    load("wi", wi_hbm, wi_v)
    load("wf", wf_hbm, wf_v)
    for r in range(1, nt):
        load("x%d" % r, x_hbm.at[chunk(r)], x_v.at[chunk(r)])
    load("v", wv_hbm, w_v.at[1])

    bar = pltpu.get_barrier_semaphore()

    def greet(device):
        pl.semaphore_signal(bar, inc=1, device_id=device, device_id_type=MESH)

    def turn(dy, dc):
        return {"y": lax.rem(y + dy, ny), "c": lax.rem(c + dc, nc)}

    for d in range(1, nt):
        greet({"tp": lax.rem(t + d, nt)})
    for dy, dc in plane:
        greet(turn(dy, dc))
    greet(before)
    for zz in range(nz - 1):

        @pl.when(zz < z)
        def _():
            greet({"z": zz})

    def remote(src, dst, send, recv, device):
        return pltpu.make_async_remote_copy(
            src_ref=src, dst_ref=dst, send_sem=send, recv_sem=recv, device_id=device, device_id_type=MESH
        )

    need("wi", "wf")
    wg_t = jnp.concatenate([wi_v[...].astype(F32), wf_v[...].astype(F32)], axis=0).astype(BF16)
    for r in range(nt):
        need("x%d" % r)
        if r == 0:
            need("k")
        if r == 1:
            load("cg", wcg_hbm, w_v.at[2])
            load("ci", wci_hbm, w_v.at[3])
            load("init", init_hbm, init_v)
        xr = x_v[chunk(r), :]
        logits = mm_nt(wg_t, xr)
        for b in range(part // BLOCK):
            gt_v[r * (part // BLOCK) + b] = logits[:, b * BLOCK : (b + 1) * BLOCK]
        k_v[chunk(r), :] = mm(xr, w_v[0]).astype(BF16)
    need("v", "init", "cg", "ci")
    load("taps", taps_hbm, taps_v)
    load("co", wco_hbm, w_v.at[4])
    load("q", wq_hbm, w_v.at[5])
    load("og", wog_hbm, w_v.at[6])
    load("gain", gain_hbm, gain_v)
    load("cout", wcout_hbm, wcout_v)
    load("mo", wmo_hbm, wmo_v)

    def conv_input(xr):
        gate = mm(xr, w_v[2]).astype(BF16)
        inp = mm(xr, w_v[3]).astype(BF16)
        return (gate.astype(F32) * inp.astype(F32)).astype(BF16).astype(F32)

    edge_v[...] = conv_input(x_v[tokens - 16 : tokens, :])

    n_gate = gt_v.shape[1] // 2
    n_row = heads * nb
    for h in range(heads):
        for b in range(nb):
            row = h * nb + b
            rows_v[0, row : row + 1, :] = gt_v[b, pl.ds(t * heads + h, 1), :]
            rows_v[1, row : row + 1, :] = gt_v[b, pl.ds(n_gate + t * heads + h, 1), :] + fb[h] + fs[h, b]
    shape = (n_row, BLOCK)
    lane = lax.broadcasted_iota(jnp.int32, shape, 1)
    in_gate = rows_v[0]
    logit = rows_v[1]
    cum = jnp.minimum(logit, 0.0) - jnp.log1p(jnp.exp(-jnp.abs(logit)))
    step = 1
    while step < BLOCK:
        cum = cum + jnp.where(lane >= step, pltpu.roll(cum, step, 1), 0.0)
        step *= 2
    lead = in_gate - cum
    high = lead
    step = 1
    while step < BLOCK:
        high = jnp.maximum(high, jnp.where(lane >= step, pltpu.roll(high, step, 1), LOW))
        step *= 2
    decay = jnp.broadcast_to(cum[:, BLOCK - 1 : BLOCK], shape)
    end_log = decay - cum + in_gate
    loc_max = jnp.broadcast_to(jnp.max(end_log, axis=1, keepdims=True), shape)
    final = jnp.exp(end_log - loc_max) * scale
    rows_v[0] = decay
    rows_v[1] = loc_max
    rows_v[2] = final
    rows_v[5] = lead
    for r in range(nt):
        v_v[chunk(r), :] = mm(x_v[chunk(r), :], w_v[1]).astype(BF16)

    first = sp == 0
    states = []
    for h in range(heads):
        top = jnp.where(first, jnp.zeros((1, BLOCK), F32), jnp.full((1, BLOCK), LOW, F32))
        state = jnp.where(first, init_v[h].T, jnp.zeros((dh, dh), F32))
        states.append((state, top, jnp.zeros((1, BLOCK), F32)))
    for b in range(nb):
        rows = slice(b * BLOCK, (b + 1) * BLOCK)
        for h in range(heads):
            head = slice(h * dh, (h + 1) * dh)
            row = h * nb + b
            state, top, past = states[h]
            pref_v[row] = state.astype(BF16)
            rows_v[3, row : row + 1, :] = top
            rows_v[4, row : row + 1, :] = past
            value_t = v_v[rows, head].astype(F32).T
            vt_v[row] = value_t.astype(BF16)
            within = mm((value_t * rows_v[2, row : row + 1, :]).astype(BF16), k_v[rows, head])
            states[h] = merge(states[h], (within, rows_v[1, row : row + 1, :], rows_v[0, row : row + 1, :]))
    for h in range(heads):
        pack(msg_v.at[h], states[h])

    spot = y * nc + c
    pl.semaphore_wait(bar, (nt - 1) + len(plane) + 1 + (nz - 1 - z))
    halo = remote(edge_v.at[pl.ds(8, 8)], halo_v, one_send.at[0], one_recv.at[0], after)
    halo.start()
    started = [halo]
    for i, (dy, dc) in enumerate(plane):
        to = turn(dy, dc)
        copy = remote(msg_v.at[to["c"]], ry_v.at[spot], y_send.at[i], y_recv.at[spot], to)
        copy.start()
        started.append(copy)
    ry_v[pl.ds(spot, 1)] = msg_v[pl.ds(c, 1)]

    local_top = rows_v[3]
    peak = jnp.maximum(local_top, high)
    rows_v[6] = peak
    rows_v[7] = jnp.exp(local_top - peak)
    col_v[0:n_row, :] = rows_v[5]
    col_v[...] = col_v[...].T

    for r in range(nt):
        cin_v[pl.ds(8 + r * part, part), :] = conv_input(x_v[chunk(r), :])
    need("taps", "co", "q")
    mine_lanes = pl.ds(pl.multiple_of(t * width, width), width)
    order = (*range(1, nt), 0)

    def outgate_query(r):
        xr = x_v[chunk(r), :]
        q_v[chunk(r), :] = mm(xr, w_v[5]).astype(BF16)
        co_v[chunk(r), :] = mm(xr, w_v[4]).astype(BF16)

    outgate_query(order[0])
    for i, r in enumerate(order):
        if i + 1 < nt:
            outgate_query(order[i + 1])
        if r == 0:
            halo.wait_recv()
            cin_v[0:8, :] = jnp.where(first, jnp.zeros((8, width), F32), halo_v[...])
        strip = 64
        for k in range(0, part, strip):
            at = r * part + k
            window = cin_v[at : at + strip + 8, :]
            conv = taps_v[0:1, :] * window[6 : strip + 6]
            conv = conv + taps_v[1:2, :] * window[7 : strip + 7]
            conv = conv + taps_v[2:3, :] * window[8 : strip + 8]
            csend_v[r, k : k + strip, :] = (co_v[at : at + strip, :].astype(F32) * conv).astype(BF16)

        @pl.when(r != t)
        def _():
            remote(csend_v.at[r], crow_v.at[:, mine_lanes], c_send.at[r], c_recv.at[t], {"tp": r}).start()

    need("og", "gain")

    def output_gate(r):
        gate = jax.nn.sigmoid(mm(x_v[chunk(r), :], w_v[6]).astype(BF16).astype(F32)) * gain_v[0:1, :]
        for i in range(per):
            for h in range(heads):
                og_v[h, r * per + i] = gate[i * BLOCK : (i + 1) * BLOCK, h * dh : (h + 1) * dh].T

    output_gate(0)
    output_gate(1)

    for i, (dy, dc) in enumerate(plane):
        far = turn(dy, dc)
        slot = far["y"] * nc + far["c"]
        remote(msg_v.at[c], ry_v.at[slot], y_send.at[i], y_recv.at[slot], far).wait_recv()
    neutral = (jnp.zeros((dh, dh), F32), jnp.full((1, BLOCK), LOW, F32), jnp.zeros((1, BLOCK), F32))
    run = ahead = partner = neutral
    for i in range(ny * nc):
        run = merge(run, unpack(ry_v.at[i]))
        if i < ny * nc - 1:
            ahead = pick(i < spot, run, ahead)
            partner = pick(i < y * nc + 1 - c, run, partner)
    pack(msgr_v, run)
    for dz in sorted(range(1, nz), key=lambda d: -min(d, nz - d)):
        zz = z + dz

        @pl.when(zz < nz)
        def _():
            remote(msgr_v, rz_v.at[z], z_send.at[dz], z_recv.at[z], {"z": zz}).start()

    for k, triple in enumerate((ahead, partner)):
        ah_v[k] = triple[0]
        ahmd_v[k, 0:1, :] = triple[1]
        ahmd_v[k, 1:2, :] = triple[2]

    for r in range(2, nt):
        output_gate(r)

    causal = lax.broadcasted_iota(jnp.int32, (BLOCK, BLOCK), 0) <= lax.broadcasted_iota(jnp.int32, (BLOCK, BLOCK), 1)
    for b in range(nb):
        rows = slice(b * BLOCK, (b + 1) * BLOCK)
        for h in range(heads):
            head = slice(h * dh, (h + 1) * dh)
            row = h * nb + b
            query = q_v[rows, head]
            score = mm_nt(k_v[rows, head], query)
            logs = jnp.where(causal, col_v[:, row : row + 1] - rows_v[6, row : row + 1, :], LOW)
            weight = (score * scale * jnp.exp(logs)).astype(BF16)
            hidden = mm(vt_v[row], weight) + rows_v[7, row : row + 1, :] * mm_nt(pref_v[row], query)
            hloc_v[h, b] = hidden - jnp.mean(hidden, axis=0, keepdims=True)

    zs_v[...] = neutral[0]
    zmd_v[0:1, :] = neutral[1]
    zmd_v[1:2, :] = neutral[2]
    for zz in range(nz - 1):

        @pl.when(zz < z)
        def _():
            remote(msgr_v, rz_v.at[zz], z_send.at[0], z_recv.at[zz], {"z": zz}).wait_recv()
            zs, zm, zd = merge((zs_v[...], zmd_v[0:1, :], zmd_v[1:2, :]), unpack(rz_v.at[zz]))
            zs_v[...] = zs
            zmd_v[0:1, :] = zm
            zmd_v[1:2, :] = zd

    rows_before = (zs_v[...], zmd_v[0:1, :], zmd_v[1:2, :])
    pack(msg4_v, merge(rows_before, (ah_v[1], ahmd_v[1, 0:1, :], ahmd_v[1, 1:2, :])))
    give = remote(msg4_v, r4_v, one_send.at[1], one_recv.at[1], {"c": 1 - c})
    give.start()
    started.append(give)
    entering = merge(rows_before, (ah_v[0], ahmd_v[0, 0:1, :], ahmd_v[0, 1:2, :]))

    def prepare(k, g, triple):
        state, top, _ = triple
        bd_v[k] = (state - jnp.mean(state, axis=0, keepdims=True)).astype(BF16)
        rows = pl.ds(pl.multiple_of(g * nb, nb), nb)
        peak = rows_v[6, rows, :]
        carry = rows_v[4, rows, :] + top
        joint = jnp.maximum(peak, carry)
        fac_v[k, 0] = jnp.exp(peak - joint)
        fac_v[k, 1] = jnp.exp(carry - joint)

    def output(k, g, d):
        r = lax.rem(t + d, nt)
        rows = pl.ds(pl.multiple_of(r * part, part), part)
        head = pl.ds(pl.multiple_of(g * dh, dh), dh)
        carried = mm_nt(bd_v[k], q_v[rows, head])
        for i in range(per):
            b = r * per + i
            hidden = fac_v[k, 0, pl.ds(b, 1), :] * hloc_v[g, b]
            hidden = hidden + fac_v[k, 1, pl.ds(b, 1), :] * carried[:, i * BLOCK : (i + 1) * BLOCK]
            spread = jnp.mean(hidden * hidden, axis=0, keepdims=True)
            out = og_v[g, b] * (hidden * lax.rsqrt(spread + EPS))
            msend_v[d, g, i * BLOCK : (i + 1) * BLOCK, :] = out.T.astype(BF16)
        if d:
            copy = remote(msend_v.at[d, g], mrow_v.at[t, g], m_send.at[d, g], m_recv.at[t, g], {"tp": r})
            copy.start()
            started.append(copy)

    prepare(0, c, entering)
    for d in near:
        output(0, c, d)
    give.wait_recv()
    prepare(1, 1 - c, unpack(r4_v))
    for d in near:
        output(1, 1 - c, d)
    output(0, c, 0)
    output(1, 1 - c, 0)

    need("cout", "mo")
    for d in near:
        r = lax.rem(t + d, nt)
        lanes = pl.ds(pl.multiple_of(r * width, width), width)
        remote(csend_v.at[r], crow_v.at[:, lanes], c_send.at[r], c_recv.at[r], {"tp": r}).wait_recv()
    crow_v[:, mine_lanes] = csend_v[t]
    tile = min(512, acc_v.shape[1])
    tiles = [slice(n * tile, (n + 1) * tile) for n in range(acc_v.shape[1] // tile)]

    def weight_rows(r):
        return pl.ds(pl.multiple_of(r * width, width), width)

    def both(ref, k):
        return jnp.concatenate([ref[k, h] for h in range(heads)], axis=1)

    for cols in tiles:
        acc_v[:, cols] = mm(crow_v[...], wcout_v[:, cols]) + mm(both(msend_v, 0), wmo_v[weight_rows(t), cols])
    for k, d in enumerate(near):
        r = lax.rem(t + d, nt)
        for h in range(heads):
            remote(msend_v.at[d, h], mrow_v.at[r, h], m_send.at[d, h], m_recv.at[r, h], {"tp": r}).wait_recv()
        for cols in tiles:
            total = acc_v[:, cols] + mm(both(mrow_v, r), wmo_v[weight_rows(r), cols])
            if k == len(near) - 1:
                out_v[:, cols] = total.astype(BF16)
            else:
                acc_v[:, cols] = total

    for copy in started:
        copy.wait_send()
    for r in range(nt):

        @pl.when(r != t)
        def _():
            remote(csend_v.at[r], crow_v.at[:, mine_lanes], c_send.at[r], c_recv.at[t], {"tp": r}).wait_send()

    for dz in range(1, nz):
        zz = z + dz

        @pl.when(zz < nz)
        def _():
            remote(msgr_v, rz_v.at[z], z_send.at[dz], z_recv.at[z], {"z": zz}).wait_send()


def per_device(sizes, layer_input, query_weight, key_weight, value_weight, outgate_weight, ingate_weight,
               forget_weight, forget_bias, forget_shift, init_state, head_gain, conv_gate_weight,
               conv_input_weight, conv_outgate_weight, conv_taps, memory_out_weight, conv_out_weight):
    nz, ny, nc, nt = sizes
    tokens, model = layer_input.shape
    width = query_weight.shape[1]
    heads, dh, _ = init_state.shape
    gates = ingate_weight.shape[1]
    nb = tokens // BLOCK
    part = tokens // nt
    channels = memory_out_weight.shape[0]
    out_width = memory_out_weight.shape[1]
    n_row = heads * nb
    dma = pltpu.SemaphoreType.DMA
    vm = pltpu.VMEM
    msg = (dh + TAIL, dh)
    scratch = [
        vm((tokens, model), BF16), vm((7, model, width), BF16), vm((gates, model), BF16), vm((gates, model), BF16),
        vm((heads, dh, dh), F32), vm((1, width), F32), vm(conv_taps.shape, F32),
        vm((channels, out_width), BF16), vm((channels, out_width), BF16),
        vm((tokens, width), BF16), vm((tokens, width), BF16), vm((tokens, width), BF16), vm((tokens, width), BF16),
        vm((heads, nb, dh, BLOCK), F32), vm((tokens + 8, width), F32), vm((heads, nb, dh, BLOCK), F32),
        vm((part, out_width), F32),
        vm((nb, 2 * gates, BLOCK), F32), vm((8, n_row, BLOCK), F32), vm((BLOCK, BLOCK), F32),
        vm((heads, 2, nb, BLOCK), F32), vm((n_row, dh, dh), BF16), vm((n_row, dh, dh), BF16), vm((heads, dh, dh), BF16),
        vm((16, width), F32), vm((8, width), F32), vm((heads, *msg), BF16), vm((ny * nc, *msg), BF16), vm(msg, BF16),
        vm((nz, *msg), BF16), vm((dh, dh), F32), vm((8, dh), F32), vm(msg, BF16), vm(msg, BF16),
        vm((heads, dh, dh), F32), vm((heads, 8, dh), F32),
        vm((nt, part, width), BF16), vm((part, channels), BF16),
        vm((nt, heads, part, dh), BF16), vm((nt, heads, part, dh), BF16),
        dma((24,)), dma((2,)), dma((2,)), dma((ny * nc,)), dma((ny * nc,)), dma((nz,)), dma((nz,)),
        dma((nt,)), dma((nt,)), dma((nt, heads)), dma((nt, heads)),
    ]
    anywhere = pl.BlockSpec(memory_space=pltpu.HBM)
    smem = pl.BlockSpec(memory_space=pltpu.SMEM)
    return pl.pallas_call(
        functools.partial(kernel, sizes),
        out_shape=pltpu.VMEM((part, out_width), BF16),
        in_specs=[anywhere] * 10 + [smem] * 2 + [anywhere] * 5,
        out_specs=pl.BlockSpec(memory_space=pltpu.VMEM),
        scratch_shapes=scratch,
        compiler_params=pltpu.CompilerParams(
            collective_id=0, has_side_effects=True, vmem_limit_bytes=65994752
        ),
    )(layer_input, key_weight, value_weight, conv_gate_weight, conv_input_weight, conv_outgate_weight,
      query_weight, outgate_weight, ingate_weight.T, forget_weight.T, forget_bias, forget_shift.T, init_state,
      head_gain.reshape(1, -1), conv_taps, memory_out_weight, conv_out_weight)


def build(mesh, sizes):
    finer = Mesh(mesh.devices.reshape(sizes), AXES)
    sp = AXES[:3]
    in_specs = (
        P(sp, None), P(None, "tp"), P(None, "tp"), P(None, "tp"), P(None, "tp"), P(), P(), P("tp"), P(sp, "tp"),
        P("tp", None, None), P("tp"), P(None, "tp"), P(None, "tp"), P(None, "tp"), P(None, "tp"), P(), P(),
    )
    return jax.shard_map(
        functools.partial(per_device, sizes), mesh=finer, in_specs=in_specs, out_specs=P(AXES, None), check_vma=False
    )


def solution(mesh):
    return build(mesh, (4, 4, 2, mesh.shape["tp"]))
```

```python
import functools

import jax
import jax.numpy as jnp
from jax import lax
from jax.experimental import pallas as pl
from jax.experimental.pallas import tpu as pltpu
from jax.sharding import Mesh
from jax.sharding import PartitionSpec as P

F32, BF16 = jnp.float32, jnp.bfloat16
MESH = pl.DeviceIdType.MESH
BLOCK = 128
EPS = 1e-05
LOW = -1e30
TAIL = 16
AXES = ("z", "y", "c", "tp")


def mm(a, b):
    return jnp.dot(a, b, preferred_element_type=F32)


def mm_nt(a, b):
    return lax.dot_general(a, b, (((1,), (1,)), ((), ())), preferred_element_type=F32)


def merge(earlier, latter):
    e_s, e_m, e_d = earlier
    l_s, l_m, l_d = latter
    top = jnp.maximum(l_d + e_m, l_m)
    return jnp.exp(l_d + e_m - top) * e_s + jnp.exp(l_m - top) * l_s, top, e_d + l_d


def pick(cond, a, b):
    return tuple(jnp.where(cond, u, v) for u, v in zip(a, b))


def thirds(v):
    hi = v.astype(BF16).astype(F32)
    mid = (v - hi).astype(BF16).astype(F32)
    return hi, mid, v - hi - mid


def pack(ref, triple):
    s, m, d = triple
    dk, lanes = s.shape
    row = lax.broadcasted_iota(jnp.int32, (TAIL, lanes), 0)
    tail = jnp.zeros((TAIL, lanes), F32)
    for k, part in enumerate((*thirds(m), *thirds(d))):
        tail = jnp.where(row == k, part, tail)
    ref[0:dk, :] = s.astype(BF16)
    ref[dk : dk + TAIL, :] = tail.astype(BF16)


def unpack(ref):
    dk = ref.shape[0] - TAIL
    tail = ref[dk : dk + TAIL, :].astype(F32)
    m = tail[0:1] + tail[1:2] + tail[2:3]
    d = tail[3:4] + tail[4:5] + tail[5:6]
    return ref[0:dk, :].astype(F32), m, d


def kernel(sizes, *refs):
    nz, ny, nc, nt = sizes
    (x_hbm, wk_hbm, wv_hbm, wcg_hbm, wci_hbm, wco_hbm, wq_hbm, wog_hbm, wi_hbm, wf_hbm,
     fb, fs, init_hbm, gain_hbm, taps_hbm, wmo_hbm, wcout_hbm, out_v) = refs[:18]
    (x_v, w_v, wi_v, wf_v, init_v, gain_v, taps_v, wmo_v, wcout_v,
     k_v, v_v, q_v, co_v, og_v, cin_v, hloc_v, acc_v,
     gt_v, rows_v, col_v, fac_v, vt_v, pref_v, bd_v,
     edge_v, halo_v, msg_v, ry_v, msgr_v, rz_v, zs_v, zmd_v, msg4_v, r4_v, ah_v, ahmd_v,
     csend_v, crow_v, msend_v, mrow_v,
     ld_sem, one_send, one_recv, y_send, y_recv, z_send, z_recv,
     c_send, c_recv, e_send, e_recv, m_send, m_recv) = refs[18:]

    z, y, c, t = (lax.axis_index(a) for a in AXES)
    n_sp = nz * ny * nc
    sp = (z * ny + y) * nc + c

    def at_sp(index):
        return {"z": lax.div(index, ny * nc), "y": lax.rem(lax.div(index, nc), ny), "c": lax.rem(index, nc)}

    after = at_sp(lax.rem(sp + 1, n_sp))
    before = at_sp(lax.rem(sp + n_sp - 1, n_sp))
    tokens = x_v.shape[0]
    part = tokens // nt
    nb = tokens // BLOCK
    width = k_v.shape[1]
    heads = width // BLOCK
    dh = BLOCK
    scale = dh ** -0.5
    per = part // BLOCK
    near = sorted(range(1, nt), key=lambda d: -min(d, nt - d))
    plane = [(dy, dc) for dy in (*sorted(range(1, ny), key=lambda d: -min(d, ny - d)), 0) for dc in range(nc) if dy or dc]

    def chunk(r):
        return pl.ds(r * part, part)

    loads = {}

    def load(name, src, dst):
        copy = pltpu.make_async_copy(src, dst, ld_sem.at[len(loads)])
        copy.start()
        loads[name] = copy

    def need(*names):
        for name in names:
            loads[name].wait()

    load("x0", x_hbm.at[chunk(0)], x_v.at[chunk(0)])
    load("k", wk_hbm, w_v.at[0])
    load("wi", wi_hbm, wi_v)
    load("wf", wf_hbm, wf_v)
    for r in range(1, nt):
        load("x%d" % r, x_hbm.at[chunk(r)], x_v.at[chunk(r)])
    load("v", wv_hbm, w_v.at[1])

    bar = pltpu.get_barrier_semaphore()

    def greet(device):
        pl.semaphore_signal(bar, inc=1, device_id=device, device_id_type=MESH)

    def turn(dy, dc):
        return {"y": lax.rem(y + dy, ny), "c": lax.rem(c + dc, nc)}

    for d in range(1, nt):
        greet({"tp": lax.rem(t + d, nt)})
    for dy, dc in plane:
        greet(turn(dy, dc))
    greet(before)
    for zz in range(nz - 1):

        @pl.when(zz < z)
        def _():
            greet({"z": zz})

    def remote(src, dst, send, recv, device):
        return pltpu.make_async_remote_copy(
            src_ref=src, dst_ref=dst, send_sem=send, recv_sem=recv, device_id=device, device_id_type=MESH
        )

    need("wi", "wf")
    wg_t = jnp.concatenate([wi_v[...].astype(F32), wf_v[...].astype(F32)], axis=0).astype(BF16)
    for r in range(nt):
        need("x%d" % r)
        if r == 0:
            need("k")
        if r == 1:
            load("cg", wcg_hbm, w_v.at[2])
            load("ci", wci_hbm, w_v.at[3])
            load("init", init_hbm, init_v)
        xr = x_v[chunk(r), :]
        logits = mm_nt(wg_t, xr)
        for b in range(part // BLOCK):
            gt_v[r * (part // BLOCK) + b] = logits[:, b * BLOCK : (b + 1) * BLOCK]
        k_v[chunk(r), :] = mm(xr, w_v[0]).astype(BF16)
    need("v", "init", "cg", "ci")
    load("taps", taps_hbm, taps_v)
    load("co", wco_hbm, w_v.at[4])
    load("q", wq_hbm, w_v.at[5])
    load("og", wog_hbm, w_v.at[6])
    load("gain", gain_hbm, gain_v)
    load("cout", wcout_hbm, wcout_v)
    load("mo", wmo_hbm, wmo_v)

    def conv_input(xr):
        gate = mm(xr, w_v[2]).astype(BF16)
        inp = mm(xr, w_v[3]).astype(BF16)
        return (gate.astype(F32) * inp.astype(F32)).astype(BF16).astype(F32)

    edge_v[...] = conv_input(x_v[tokens - 16 : tokens, :])

    n_gate = gt_v.shape[1] // 2
    n_row = heads * nb
    for h in range(heads):
        for b in range(nb):
            row = h * nb + b
            rows_v[0, row : row + 1, :] = gt_v[b, pl.ds(t * heads + h, 1), :]
            rows_v[1, row : row + 1, :] = gt_v[b, pl.ds(n_gate + t * heads + h, 1), :] + fb[h] + fs[h, b]
    shape = (n_row, BLOCK)
    lane = lax.broadcasted_iota(jnp.int32, shape, 1)
    in_gate = rows_v[0]
    logit = rows_v[1]
    cum = jnp.minimum(logit, 0.0) - jnp.log1p(jnp.exp(-jnp.abs(logit)))
    step = 1
    while step < BLOCK:
        cum = cum + jnp.where(lane >= step, pltpu.roll(cum, step, 1), 0.0)
        step *= 2
    lead = in_gate - cum
    high = lead
    step = 1
    while step < BLOCK:
        high = jnp.maximum(high, jnp.where(lane >= step, pltpu.roll(high, step, 1), LOW))
        step *= 2
    decay = jnp.broadcast_to(cum[:, BLOCK - 1 : BLOCK], shape)
    end_log = decay - cum + in_gate
    loc_max = jnp.broadcast_to(jnp.max(end_log, axis=1, keepdims=True), shape)
    final = jnp.exp(end_log - loc_max) * scale
    rows_v[0] = decay
    rows_v[1] = loc_max
    rows_v[2] = final
    rows_v[5] = lead
    for r in range(nt):
        v_v[chunk(r), :] = mm(x_v[chunk(r), :], w_v[1]).astype(BF16)

    first = sp == 0
    states = []
    for h in range(heads):
        top = jnp.where(first, jnp.zeros((1, BLOCK), F32), jnp.full((1, BLOCK), LOW, F32))
        state = jnp.where(first, init_v[h].T, jnp.zeros((dh, dh), F32))
        states.append((state, top, jnp.zeros((1, BLOCK), F32)))
    for b in range(nb):
        rows = slice(b * BLOCK, (b + 1) * BLOCK)
        for h in range(heads):
            head = slice(h * dh, (h + 1) * dh)
            row = h * nb + b
            state, top, past = states[h]
            pref_v[row] = state.astype(BF16)
            rows_v[3, row : row + 1, :] = top
            rows_v[4, row : row + 1, :] = past
            value_t = v_v[rows, head].astype(F32).T
            vt_v[row] = value_t.astype(BF16)
            within = mm((value_t * rows_v[2, row : row + 1, :]).astype(BF16), k_v[rows, head])
            states[h] = merge(states[h], (within, rows_v[1, row : row + 1, :], rows_v[0, row : row + 1, :]))
    for h in range(heads):
        pack(msg_v.at[h], states[h])

    spot = y * nc + c
    pl.semaphore_wait(bar, (nt - 1) + len(plane) + 1 + (nz - 1 - z))
    halo = remote(edge_v.at[pl.ds(8, 8)], halo_v, one_send.at[0], one_recv.at[0], after)
    halo.start()
    started = [halo]
    for i, (dy, dc) in enumerate(plane):
        to = turn(dy, dc)
        copy = remote(msg_v.at[to["c"]], ry_v.at[spot], y_send.at[i], y_recv.at[spot], to)
        copy.start()
        started.append(copy)
    ry_v[pl.ds(spot, 1)] = msg_v[pl.ds(c, 1)]

    local_top = rows_v[3]
    peak = jnp.maximum(local_top, high)
    rows_v[6] = peak
    rows_v[7] = jnp.exp(local_top - peak)
    col_v[0:n_row, :] = rows_v[5]
    col_v[...] = col_v[...].T

    for r in range(nt):
        cin_v[pl.ds(8 + r * part, part), :] = conv_input(x_v[chunk(r), :])
    need("taps", "co", "q")
    mine_lanes = pl.ds(pl.multiple_of(t * width, width), width)
    order = [lax.rem(t + d, nt) for d in (*near, 0)]
    cin_v[0:8, :] = jnp.zeros((8, width), F32)

    def outgate_query(r):
        rows = pl.ds(pl.multiple_of(r * part, part), part)
        xr = x_v[rows, :]
        q_v[rows, :] = mm(xr, w_v[5]).astype(BF16)
        co_v[rows, :] = mm(xr, w_v[4]).astype(BF16)

    def convolve(at, n):
        window = cin_v[pl.ds(at, n + 8), :]
        conv = taps_v[0:1, :] * window[6 : n + 6]
        conv = conv + taps_v[1:2, :] * window[7 : n + 7]
        conv = conv + taps_v[2:3, :] * window[8 : n + 8]
        return (co_v[pl.ds(at, n), :].astype(F32) * conv).astype(BF16)

    def conv_copy(r, source, rows, recv):
        lanes = pl.ds(pl.multiple_of(source * width, width), width)
        return remote(csend_v.at[r, rows], crow_v.at[rows, lanes], c_send.at[r], recv, {"tp": r})

    whole = pl.ds(0, part)
    later = pl.ds(16, part - 16)
    early = pl.ds(0, 16)

    outgate_query(order[0])
    for i, r in enumerate(order):
        if i + 1 < nt:
            outgate_query(order[i + 1])
        strip = 64
        for k in range(0, part, strip):
            csend_v[r, k : k + strip, :] = convolve(pl.multiple_of(r * part + k, strip), strip)
        if i + 1 < nt:

            @pl.when(r != 0)
            def _():
                conv_copy(r, t, whole, c_recv.at[t]).start()

            @pl.when(r == 0)
            def _():
                conv_copy(r, t, later, c_recv.at[t]).start()

    need("og", "gain")

    def output_gate(r):
        gate = jax.nn.sigmoid(mm(x_v[chunk(r), :], w_v[6]).astype(BF16).astype(F32)) * gain_v[0:1, :]
        for i in range(per):
            for h in range(heads):
                og_v[h, r * per + i] = gate[i * BLOCK : (i + 1) * BLOCK, h * dh : (h + 1) * dh].T

    output_gate(0)
    output_gate(1)

    for i, (dy, dc) in enumerate(plane):
        far = turn(dy, dc)
        slot = far["y"] * nc + far["c"]
        remote(msg_v.at[c], ry_v.at[slot], y_send.at[i], y_recv.at[slot], far).wait_recv()
    neutral = (jnp.zeros((dh, dh), F32), jnp.full((1, BLOCK), LOW, F32), jnp.zeros((1, BLOCK), F32))
    run = ahead = partner = neutral
    for i in range(ny * nc):
        run = merge(run, unpack(ry_v.at[i]))
        if i < ny * nc - 1:
            ahead = pick(i < spot, run, ahead)
            partner = pick(i < y * nc + 1 - c, run, partner)
    pack(msgr_v, run)
    for dz in sorted(range(1, nz), key=lambda d: -min(d, nz - d)):
        zz = z + dz

        @pl.when(zz < nz)
        def _():
            remote(msgr_v, rz_v.at[z], z_send.at[dz], z_recv.at[z], {"z": zz}).start()

    for k, triple in enumerate((ahead, partner)):
        ah_v[k] = triple[0]
        ahmd_v[k, 0:1, :] = triple[1]
        ahmd_v[k, 1:2, :] = triple[2]

    halo.wait_recv()
    cin_v[0:8, :] = jnp.where(first, jnp.zeros((8, width), F32), halo_v[...])
    csend_v[0, 0:16, :] = convolve(0, 16)

    def edge_copy(source):
        lanes = pl.ds(pl.multiple_of(source * width, width), width)
        return remote(csend_v.at[0, early], crow_v.at[early, lanes], e_send.at[0], e_recv.at[source], {"tp": 0})

    @pl.when(t != 0)
    def _():
        edge_copy(t).start()

    for r in range(2, nt):
        output_gate(r)

    causal = lax.broadcasted_iota(jnp.int32, (BLOCK, BLOCK), 0) <= lax.broadcasted_iota(jnp.int32, (BLOCK, BLOCK), 1)
    for b in range(nb):
        rows = slice(b * BLOCK, (b + 1) * BLOCK)
        for h in range(heads):
            head = slice(h * dh, (h + 1) * dh)
            row = h * nb + b
            query = q_v[rows, head]
            score = mm_nt(k_v[rows, head], query)
            logs = jnp.where(causal, col_v[:, row : row + 1] - rows_v[6, row : row + 1, :], LOW)
            weight = (score * scale * jnp.exp(logs)).astype(BF16)
            hidden = mm(vt_v[row], weight) + rows_v[7, row : row + 1, :] * mm_nt(pref_v[row], query)
            hloc_v[h, b] = hidden - jnp.mean(hidden, axis=0, keepdims=True)

    zs_v[...] = neutral[0]
    zmd_v[0:1, :] = neutral[1]
    zmd_v[1:2, :] = neutral[2]
    for zz in range(nz - 1):

        @pl.when(zz < z)
        def _():
            remote(msgr_v, rz_v.at[zz], z_send.at[0], z_recv.at[zz], {"z": zz}).wait_recv()
            zs, zm, zd = merge((zs_v[...], zmd_v[0:1, :], zmd_v[1:2, :]), unpack(rz_v.at[zz]))
            zs_v[...] = zs
            zmd_v[0:1, :] = zm
            zmd_v[1:2, :] = zd

    rows_before = (zs_v[...], zmd_v[0:1, :], zmd_v[1:2, :])
    pack(msg4_v, merge(rows_before, (ah_v[1], ahmd_v[1, 0:1, :], ahmd_v[1, 1:2, :])))
    give = remote(msg4_v, r4_v, one_send.at[1], one_recv.at[1], {"c": 1 - c})
    give.start()
    started.append(give)
    entering = merge(rows_before, (ah_v[0], ahmd_v[0, 0:1, :], ahmd_v[0, 1:2, :]))

    def prepare(k, g, triple):
        state, top, _ = triple
        bd_v[k] = (state - jnp.mean(state, axis=0, keepdims=True)).astype(BF16)
        rows = pl.ds(pl.multiple_of(g * nb, nb), nb)
        peak = rows_v[6, rows, :]
        carry = rows_v[4, rows, :] + top
        joint = jnp.maximum(peak, carry)
        fac_v[k, 0] = jnp.exp(peak - joint)
        fac_v[k, 1] = jnp.exp(carry - joint)

    def output(k, g, d):
        r = lax.rem(t + d, nt)
        rows = pl.ds(pl.multiple_of(r * part, part), part)
        head = pl.ds(pl.multiple_of(g * dh, dh), dh)
        carried = mm_nt(bd_v[k], q_v[rows, head])
        for i in range(per):
            b = r * per + i
            hidden = fac_v[k, 0, pl.ds(b, 1), :] * hloc_v[g, b]
            hidden = hidden + fac_v[k, 1, pl.ds(b, 1), :] * carried[:, i * BLOCK : (i + 1) * BLOCK]
            spread = jnp.mean(hidden * hidden, axis=0, keepdims=True)
            out = og_v[g, b] * (hidden * lax.rsqrt(spread + EPS))
            msend_v[d, g, i * BLOCK : (i + 1) * BLOCK, :] = out.T.astype(BF16)
        if d:
            copy = remote(msend_v.at[d, g], mrow_v.at[t, g], m_send.at[d, g], m_recv.at[t, g], {"tp": r})
            copy.start()
            started.append(copy)

    prepare(0, c, entering)
    for d in near:
        output(0, c, d)
    output(0, c, 0)
    give.wait_recv()
    prepare(1, 1 - c, unpack(r4_v))
    for d in near:
        output(1, 1 - c, d)
    output(1, 1 - c, 0)

    need("cout", "mo")
    for d in near:
        r = lax.rem(t + d, nt)

        @pl.when(t != 0)
        def _():
            conv_copy(0, r, whole, c_recv.at[r]).wait_recv()

        @pl.when(t == 0)
        def _():
            conv_copy(0, r, later, c_recv.at[r]).wait_recv()
            edge_copy(r).wait_recv()

    crow_v[:, mine_lanes] = csend_v[t]
    tile = min(512, acc_v.shape[1])
    tiles = [slice(n * tile, (n + 1) * tile) for n in range(acc_v.shape[1] // tile)]

    def weight_rows(r):
        return pl.ds(pl.multiple_of(r * width, width), width)

    def both(ref, k):
        return jnp.concatenate([ref[k, h] for h in range(heads)], axis=1)

    for cols in tiles:
        acc_v[:, cols] = mm(crow_v[...], wcout_v[:, cols]) + mm(both(msend_v, 0), wmo_v[weight_rows(t), cols])
    for k, d in enumerate(near):
        r = lax.rem(t + d, nt)
        for h in range(heads):
            remote(msend_v.at[d, h], mrow_v.at[r, h], m_send.at[d, h], m_recv.at[r, h], {"tp": r}).wait_recv()
        for cols in tiles:
            total = acc_v[:, cols] + mm(both(mrow_v, r), wmo_v[weight_rows(r), cols])
            if k == len(near) - 1:
                out_v[:, cols] = total.astype(BF16)
            else:
                acc_v[:, cols] = total

    for copy in started:
        copy.wait_send()
    for r in order[:-1]:

        @pl.when(r != 0)
        def _():
            conv_copy(r, t, whole, c_recv.at[t]).wait_send()

        @pl.when(r == 0)
        def _():
            conv_copy(r, t, later, c_recv.at[t]).wait_send()
            edge_copy(t).wait_send()

    for dz in range(1, nz):
        zz = z + dz

        @pl.when(zz < nz)
        def _():
            remote(msgr_v, rz_v.at[z], z_send.at[dz], z_recv.at[z], {"z": zz}).wait_send()


def per_device(sizes, layer_input, query_weight, key_weight, value_weight, outgate_weight, ingate_weight,
               forget_weight, forget_bias, forget_shift, init_state, head_gain, conv_gate_weight,
               conv_input_weight, conv_outgate_weight, conv_taps, memory_out_weight, conv_out_weight):
    nz, ny, nc, nt = sizes
    tokens, model = layer_input.shape
    width = query_weight.shape[1]
    heads, dh, _ = init_state.shape
    gates = ingate_weight.shape[1]
    nb = tokens // BLOCK
    part = tokens // nt
    channels = memory_out_weight.shape[0]
    out_width = memory_out_weight.shape[1]
    n_row = heads * nb
    dma = pltpu.SemaphoreType.DMA
    vm = pltpu.VMEM
    msg = (dh + TAIL, dh)
    scratch = [
        vm((tokens, model), BF16), vm((7, model, width), BF16), vm((gates, model), BF16), vm((gates, model), BF16),
        vm((heads, dh, dh), F32), vm((1, width), F32), vm(conv_taps.shape, F32),
        vm((channels, out_width), BF16), vm((channels, out_width), BF16),
        vm((tokens, width), BF16), vm((tokens, width), BF16), vm((tokens, width), BF16), vm((tokens, width), BF16),
        vm((heads, nb, dh, BLOCK), F32), vm((tokens + 8, width), F32), vm((heads, nb, dh, BLOCK), F32),
        vm((part, out_width), F32),
        vm((nb, 2 * gates, BLOCK), F32), vm((8, n_row, BLOCK), F32), vm((BLOCK, BLOCK), F32),
        vm((heads, 2, nb, BLOCK), F32), vm((n_row, dh, dh), BF16), vm((n_row, dh, dh), BF16), vm((heads, dh, dh), BF16),
        vm((16, width), F32), vm((8, width), F32), vm((heads, *msg), BF16), vm((ny * nc, *msg), BF16), vm(msg, BF16),
        vm((nz, *msg), BF16), vm((dh, dh), F32), vm((8, dh), F32), vm(msg, BF16), vm(msg, BF16),
        vm((heads, dh, dh), F32), vm((heads, 8, dh), F32),
        vm((nt, part, width), BF16), vm((part, channels), BF16),
        vm((nt, heads, part, dh), BF16), vm((nt, heads, part, dh), BF16),
        dma((24,)), dma((2,)), dma((2,)), dma((ny * nc,)), dma((ny * nc,)), dma((nz,)), dma((nz,)),
        dma((nt,)), dma((nt,)), dma((1,)), dma((nt,)), dma((nt, heads)), dma((nt, heads)),
    ]
    anywhere = pl.BlockSpec(memory_space=pltpu.HBM)
    smem = pl.BlockSpec(memory_space=pltpu.SMEM)
    return pl.pallas_call(
        functools.partial(kernel, sizes),
        out_shape=pltpu.VMEM((part, out_width), BF16),
        in_specs=[anywhere] * 10 + [smem] * 2 + [anywhere] * 5,
        out_specs=pl.BlockSpec(memory_space=pltpu.VMEM),
        scratch_shapes=scratch,
        compiler_params=pltpu.CompilerParams(
            collective_id=0, has_side_effects=True, vmem_limit_bytes=65994752
        ),
    )(layer_input, key_weight, value_weight, conv_gate_weight, conv_input_weight, conv_outgate_weight,
      query_weight, outgate_weight, ingate_weight.T, forget_weight.T, forget_bias, forget_shift.T, init_state,
      head_gain.reshape(1, -1), conv_taps, memory_out_weight, conv_out_weight)


def build(mesh, sizes):
    finer = Mesh(mesh.devices.reshape(sizes), AXES)
    sp = AXES[:3]
    in_specs = (
        P(sp, None), P(None, "tp"), P(None, "tp"), P(None, "tp"), P(None, "tp"), P(), P(), P("tp"), P(sp, "tp"),
        P("tp", None, None), P("tp"), P(None, "tp"), P(None, "tp"), P(None, "tp"), P(None, "tp"), P(), P(),
    )
    return jax.shard_map(
        functools.partial(per_device, sizes), mesh=finer, in_specs=in_specs, out_specs=P(AXES, None), check_vma=False
    )


def solution(mesh):
    return build(mesh, (4, 4, 2, mesh.shape["tp"]))
```
